32 devices in a mesh: dp: 4 (over y, x), kv: 4 (over z), tp: 2 (over core).
Axes of the slice: x: 2, y: 2, z: 4, core: 2. Of those that a mesh axis runs over, the one named last changes fastest.
Arguments:
- tokens: bfloat16 [4096, 2048], P(('dp', 'kv')), parts along dimension 0, may hold values from -7.5 to 7.5
- chosen: int32 [32, 32], P('dp'), parts along dimension 0, may hold values from -1 to 7, as said below
- w_query: bfloat16 [2048, 512], P(None, 'tp'), may hold values from -0.125 to 0.125
- w_key: bfloat16 [2048, 128], P(None, 'tp'), may hold values from -0.125 to 0.125
- w_value: bfloat16 [2048, 128], P(None, 'tp'), may hold values from -0.125 to 0.125
- w_out: bfloat16 [512, 2048], P(None, 'tp'), may hold values from -0.25 to 0.25
- q_gain: float32 [64], replicated, may hold values from 0.1 to 10.5
- k_gain: float32 [64], replicated, may hold values from 0.1 to 10.5
Outputs:
- output: bfloat16 [4096, 2048], P(('dp', 'kv'), 'tp'), parts along dimension 0
The draws below stay inside these ranges and needn't reach their ends.
There are 4 independent parts, one for each index of `dp`. The reference program is written for one: setup_inputs(seed, part) draws one part's arguments, and reference() takes and returns one part's arrays. A program takes and returns all parts, laid end to end along the dimension named above; an argument that names none is the same for every part. Nothing has to cross between parts.
Inputs may be any that keep to these rules, and one draw needn't show every extreme that they name: `chosen`: row b lists the key blocks read by query block b: its live entries come first, are distinct, at most b, and include b; the rest are -1. Over the 2 query blocks of one shard of positions, the live entries name at most one distinct key block of any other shard, and one shard reaches that.
All inputs are finite; a program needn't handle non-finite values.
Results may differ from the reference program's by a relative error of at most 0.0039.
The reference program's roundings to bfloat16 on the way (of `query`, `key`, `value`, `weights` and `attended`) count: a program that leaves them out, or rounds other values in their place, can miss the bound.
Values may be sent and summed in bfloat16 or wider, within the bound.
A program may use at most 64 MiB of HBM per device.

```python
import jax
import jax.numpy as jnp
from jax import lax

D = 2048
HEADS = 8
HD = 64
KV_HEADS = 2
BLOCK = 128
NSEL = 32
TOK_DEV = 256
SEQ = 1024
NBLK = 8


def draw_chosen(key, part):
    devices = SEQ // TOK_DEV
    per_dev = TOK_DEV // BLOCK
    nblocks = SEQ // BLOCK
    key_pop, key_rank, key_pick = jax.random.split(jax.random.fold_in(key, 11), 3)
    popular = jax.random.randint(key_pop, (devices,), 0, 3)
    noise = jax.random.randint(key_rank, (devices, devices), 0, 1 << 16)
    requester = jnp.arange(devices, dtype=jnp.int32)[:, None]
    owner_idx = jnp.arange(devices, dtype=jnp.int32)[None, :]
    forced = ((owner_idx == requester - 1) | (owner_idx == requester - devices // 2)).astype(jnp.int32)
    priority = noise + popular[None, :] * (1 << 16) + forced * (1 << 19)
    ranked = jnp.where(owner_idx < requester, priority * devices + owner_idx, -1 - owner_idx)
    _, order = lax.top_k(ranked, devices)
    offset_pick = jax.random.randint(key_pick, (devices, devices), 0, per_dev)
    picked = owner_idx * per_dev + offset_pick
    picked_sorted = jnp.take_along_axis(picked, order, axis=1)
    block_idx = jnp.arange(nblocks, dtype=jnp.int32)
    dev_of = block_idx // per_dev
    local_of = block_idx % per_dev
    slot_idx = jnp.arange(NSEL, dtype=jnp.int32)[None, :]
    remote_count = jnp.minimum(NSEL - (local_of + 1), dev_of)[:, None]
    local_entry = dev_of[:, None] * per_dev + slot_idx
    remote_pos = jnp.clip(slot_idx - (local_of[:, None] + 1), 0, devices - 1)
    remote_entry = jnp.take_along_axis(picked_sorted[dev_of], remote_pos, axis=1)
    result = jnp.where(slot_idx <= local_of[:, None], local_entry, jnp.where(slot_idx - (local_of[:, None] + 1) < remote_count, remote_entry, -1))
    return result.astype(jnp.int32)


def draw_tokens(key, part):
    base = jax.random.fold_in(key, 31)
    key_dir, key_noise = jax.random.split(base)
    direction = jnp.clip(jax.random.normal(key_dir, (D,), jnp.float32), -4.0, 4.0)
    noise = jnp.clip(jax.random.normal(key_noise, (SEQ, D), jnp.float32), -6.0, 6.0)
    amplitude = 0.3
    return (noise + amplitude * direction[None, :]).astype(jnp.bfloat16)


def gain_draw(key, which):
    own = jax.random.fold_in(key, which)
    values = 1.5 * (1.0 + 0.18 * jnp.clip(jax.random.normal(own, (HD,), jnp.float32), -5.0, 5.0))
    return values.astype(jnp.float32)


def draw_q_gain(key, part):
    return gain_draw(key, 21)


def draw_k_gain(key, part):
    return gain_draw(key, 22)


def levels(own_key, dims, cuts, least, largest):
    loudness = 1.0
    for dim, parts in cuts:
        steps = jax.random.uniform(jax.random.fold_in(jax.random.fold_in(own_key, 6), dim), (parts,), jnp.float32, least / len(cuts), largest / len(cuts))
        loudness = loudness * jnp.repeat(jnp.exp(steps), dims[dim] // parts).reshape((-1,) + (1,) * (len(dims) - 1 - dim))
    return loudness


def normal_values(stream_key, dims, deviation, most, pieces=(), kind=jnp.bfloat16):
    entries = deviation * jax.random.normal(stream_key, dims, jnp.float32)
    if pieces:
        entries = entries * levels(stream_key, dims, pieces, -0.22, 0.18)
    return jnp.clip(entries, -most, most).astype(kind)


def setup_inputs(seed: int = 0, part: int = 0) -> dict:
    splits = jax.random.split(jax.random.key(seed), 9)
    part_splits = jax.random.split(jax.random.fold_in(splits[8], part), 9)
    return {
        "tokens": draw_tokens(jax.random.fold_in(jax.random.fold_in(splits[8], part), 71), part),
        "chosen": draw_chosen(jax.random.fold_in(jax.random.fold_in(splits[8], part), 71), part),
        "w_query": normal_values(splits[2], (D, HEADS * HD), D ** -0.5, 0.125, ((1, 2),)),
        "w_key": normal_values(splits[3], (D, KV_HEADS * HD), D ** -0.5, 0.125, ((1, 2),)),
        "w_value": normal_values(splits[4], (D, KV_HEADS * HD), D ** -0.5, 0.125, ((1, 2),)),
        "w_out": normal_values(splits[5], (HEADS * HD, D), (HEADS * HD) ** -0.5, 0.25, ((1, 2),)),
        "q_gain": draw_q_gain(jax.random.fold_in(splits[8], 71), part),
        "k_gain": draw_k_gain(jax.random.fold_in(splits[8], 71), part),
    }


NEGATIVE = -1e+30
EPSILON = 1e-05

def head_norm(values, scale_vec):
    mean_sq = lax.optimization_barrier(jnp.mean(values * values, axis=-1, keepdims=True))
    return values * lax.rsqrt(mean_sq + EPSILON) * scale_vec

def reference(tokens, chosen, w_query, w_key, w_value, w_out, q_gain, k_gain):
    seq_len = tokens.shape[0]
    group = HEADS // KV_HEADS
    query = head_norm(jnp.dot(tokens, w_query, preferred_element_type=jnp.float32).reshape(seq_len, HEADS, HD), q_gain).astype(jnp.bfloat16)
    keyed = head_norm(jnp.dot(tokens, w_key, preferred_element_type=jnp.float32).reshape(seq_len, KV_HEADS, HD), k_gain).astype(jnp.bfloat16)
    value = jnp.dot(tokens, w_value, preferred_element_type=jnp.float32).astype(jnp.bfloat16).reshape(seq_len, KV_HEADS, HD)
    key_blocks = keyed.reshape(NBLK, BLOCK, KV_HEADS, HD)
    val_blocks = value.reshape(NBLK, BLOCK, KV_HEADS, HD)

    def one_block(inputs):
        queries, block_ids, block_idx = inputs
        live_ids = block_ids >= 0
        safe_ids = jnp.maximum(block_ids, 0).astype(jnp.int32)
        keyset = key_blocks[safe_ids].reshape(NSEL * BLOCK, KV_HEADS, HD).astype(jnp.float32)
        valset = val_blocks[safe_ids].reshape(NSEL * BLOCK, KV_HEADS, HD).astype(jnp.float32)
        key_pos = (safe_ids[:, None] * BLOCK + jnp.arange(BLOCK, dtype=jnp.int32)[None, :]).reshape(-1)
        live_keys = jnp.repeat(live_ids, BLOCK)
        query_pos = block_idx * BLOCK + jnp.arange(BLOCK, dtype=jnp.int32)
        allowed = live_keys[None, :] & (key_pos[None, :] <= query_pos[:, None])
        grouped = queries.reshape(BLOCK, KV_HEADS, group, HD).astype(jnp.float32)
        scores = jnp.einsum('qhgd,khd->hgqk', grouped, keyset) * HD ** (-0.5)
        scores = jnp.where(allowed[None, None], scores, NEGATIVE)
        peak = lax.optimization_barrier(jnp.max(scores, axis=-1, keepdims=True))
        expd = jnp.exp(scores - peak)
        totals = lax.optimization_barrier(jnp.sum(expd, axis=-1))
        weights = expd.astype(jnp.bfloat16).astype(jnp.float32)
        mixed = jnp.einsum('hgqk,khd->qhgd', weights, valset)
        mixed = mixed / jnp.transpose(totals, (2, 0, 1))[..., None]
        mixed = mixed.reshape(BLOCK, HEADS, HD)
        normed = head_norm(mixed, jnp.float32(1.0))
        return normed.astype(jnp.bfloat16).reshape(BLOCK, HEADS * HD)
    attended = lax.map(one_block, (query.reshape(NBLK, BLOCK, HEADS, HD), chosen, jnp.arange(NBLK, dtype=jnp.int32)))
    attended = attended.reshape(seq_len, HEADS * HD)
    return jnp.dot(attended, w_out, preferred_element_type=jnp.float32).astype(jnp.bfloat16)
```

```python
import functools

import jax
import jax.numpy as jnp
from jax import lax
from jax.experimental import pallas as pl
from jax.experimental.pallas import tpu as pltpu
from jax.sharding import PartitionSpec as P

HD = 64
BLOCK = 128
NEGATIVE = -1e30
EPSILON = 1e-05
MESH = pl.DeviceIdType.MESH
F32 = jnp.float32
BF16 = jnp.bfloat16


def repeat(count, body):
    if count <= 8:
        for i in range(count):
            body(i)
    else:
        lax.fori_loop(0, count, lambda i, c: (body(i), c)[1], 0)


def dot_nt(a, b):
    return lax.dot_general(a, b, (((1,), (1,)), ((), ())), preferred_element_type=F32)


def kernel(
    kv_n, tp_n, group,
    chosen_ref, qg_ref, kg_ref, tok_hbm, wq_hbm, wk_hbm, wv_hbm, wo_hbm,
    out_ref,
    tok, wq, wkv, wo, local, stage, slots, queries, mine, theirs,
    load_sem, kv_send, kv_recv, tp_send, tp_recv,
):
    me = lax.axis_index("kv")
    core = lax.axis_index("tp")
    rows = tok.shape[0]
    per_dev = rows // BLOCK
    q_width = wq.shape[1]
    heads = q_width // HD
    first = me * per_dev

    loads = [
        pltpu.make_async_copy(wk_hbm, wkv.at[pl.ds(0, HD)], load_sem.at[0]),
        pltpu.make_async_copy(wv_hbm, wkv.at[pl.ds(HD, HD)], load_sem.at[1]),
        pltpu.make_async_copy(tok_hbm, tok, load_sem.at[2]),
        pltpu.make_async_copy(wq_hbm, wq, load_sem.at[3]),
        pltpu.make_async_copy(wo_hbm, wo, load_sem.at[4]),
    ]
    for load in loads:
        load.start()

    barrier = pltpu.get_barrier_semaphore()

    def greet(i):
        pl.semaphore_signal(
            barrier, inc=1, device_id={"kv": lax.rem(me + i + 1, kv_n)}, device_id_type=MESH
        )

    repeat(kv_n - 1, greet)
    for r in range(1, tp_n):
        pl.semaphore_signal(
            barrier, inc=1, device_id={"tp": lax.rem(core + r, tp_n)}, device_id_type=MESH
        )

    chosen = chosen_ref[...]
    row_id = lax.broadcasted_iota(jnp.int32, chosen.shape, 0)

    def found(cond):
        return jnp.max(jnp.where(cond, 1.0, 0.0), axis=(0, 1), keepdims=True)

    for load in loads[:3]:
        load.wait()
    kv = dot_nt(tok[...], wkv[...])
    lane = lax.broadcasted_iota(jnp.int32, (rows, 2 * HD), 1)
    is_key = lane < HD
    mean_sq = jnp.sum(jnp.where(is_key, kv * kv, 0.0), axis=-1, keepdims=True) * (1.0 / HD)
    gain = jnp.concatenate([kg_ref[...], jnp.ones((1, HD), F32)], axis=1)
    packed = jnp.where(is_key, kv * lax.rsqrt(mean_sq + EPSILON), kv) * gain
    local[...] = packed.astype(BF16)

    def fill(i):
        dest = me + i + 1

        @pl.when(dest < kv_n)
        def _():
            asked = (row_id >= dest * per_dev) & (row_id < (dest + 1) * per_dev)
            sel = packed[:BLOCK]
            for j in range(1, per_dev):
                hit = jnp.broadcast_to(found(asked & (chosen == first + j)), sel.shape)
                sel = jnp.where(hit > 0.5, packed[j * BLOCK : (j + 1) * BLOCK], sel)
            stage[i] = sel.astype(BF16)

        @pl.when(me - i - 1 < 0)
        def _():
            slots[i] = jnp.zeros(slots.shape[1:], BF16)

    repeat(kv_n - 1, fill)

    pl.semaphore_wait(barrier, kv_n - 1 + tp_n - 1)

    def kv_copy(i):
        return pltpu.make_async_remote_copy(
            src_ref=stage.at[i],
            dst_ref=slots.at[i],
            send_sem=kv_send.at[i],
            recv_sem=kv_recv.at[i],
            device_id={"kv": lax.rem(me + i + 1, kv_n)},
            device_id_type=MESH,
        )

    def send(i):
        far = kv_n - 2 - i

        @pl.when(me + far + 1 < kv_n)
        def _():
            kv_copy(far).start()

    repeat(kv_n - 1, send)

    loads[3].wait()
    query = jnp.dot(tok[...], wq[...], preferred_element_type=F32)
    for h in range(heads):
        qh = query[:, h * HD : (h + 1) * HD]
        q_sq = jnp.mean(qh * qh, axis=-1, keepdims=True)
        qh = (qh * lax.rsqrt(q_sq + EPSILON) * qg_ref[...] * HD**-0.5).astype(BF16)
        qh = jnp.concatenate([qh, jnp.zeros((rows, HD), BF16)], axis=1)
        for lb in range(per_dev):
            queries[lb, h * BLOCK : (h + 1) * BLOCK] = qh[lb * BLOCK : (lb + 1) * BLOCK]

    lane_row = lax.broadcasted_iota(jnp.int32, (1, 2 * HD), 1)
    keep = jnp.where(lane_row < HD, 0.0, 1.0).astype(BF16)
    ones = jnp.where(lane_row < HD, 1.0, 0.0).astype(BF16)

    def with_ones(block):
        return block * keep + ones

    q_pos = lax.rem(
        lax.broadcasted_iota(jnp.int32, (heads * BLOCK, BLOCK), 0), BLOCK
    )
    causal = lax.broadcasted_iota(jnp.int32, (heads * BLOCK, BLOCK), 1) <= q_pos

    def bias_of(cond):
        return jnp.broadcast_to((1.0 - found(cond)) * NEGATIVE, (1, BLOCK))

    state = []
    for lb in range(per_dev):
        mine_row = row_id == first + lb
        scores = dot_nt(queries[lb], local[: (lb + 1) * BLOCK])
        parts = [
            scores[:, j * BLOCK : (j + 1) * BLOCK] + bias_of(mine_row & (chosen == first + j))
            for j in range(lb)
        ]
        parts.append(jnp.where(causal, scores[:, lb * BLOCK :], NEGATIVE))
        scores = jnp.concatenate(parts, axis=1) if lb else parts[0]
        peak = jnp.max(scores, axis=-1, keepdims=True)
        weights = jnp.exp(scores - peak).astype(BF16)
        acc = jnp.dot(
            weights, with_ones(local[: (lb + 1) * BLOCK]), preferred_element_type=F32
        )
        state.append((peak, acc))

    def arrive(i):
        @pl.when(me - i - 1 >= 0)
        def _():
            kv_copy(i).wait_recv()

    def merge(lb, base, peak, acc):
        mine_row = row_id == first + lb
        keyset = slots[pl.ds(base, group)].reshape(group * BLOCK, 2 * HD)
        biases = []
        for g in range(group):
            low = (me - base - g - 1) * per_dev
            biases.append(
                bias_of(mine_row & (chosen >= 0) & (chosen >= low) & (chosen < low + per_dev))
            )
        scores = dot_nt(queries[lb], keyset) + jnp.concatenate(biases, axis=1)
        peak_now = jnp.maximum(peak, jnp.max(scores, axis=-1, keepdims=True))
        weights = jnp.exp(scores - peak_now).astype(BF16)
        acc = acc * jnp.exp(peak - peak_now) + jnp.dot(
            weights, with_ones(keyset), preferred_element_type=F32
        )
        return peak_now, acc

    def tp_copy(r, lb):
        return pltpu.make_async_remote_copy(
            src_ref=mine.at[lb],
            dst_ref=theirs.at[r - 1, lb],
            send_sem=tp_send.at[r - 1, lb],
            recv_sem=tp_recv.at[r - 1, lb],
            device_id={"tp": lax.rem(core + r, tp_n)},
            device_id_type=MESH,
        )

    repeat(kv_n - 1, arrive)
    groups = (kv_n - 1) // group
    for lb in range(per_dev):
        peak, acc = state[lb]
        if groups <= 2:
            for n in range(groups):
                peak, acc = merge(lb, n * group, peak, acc)
        else:
            peak, acc = lax.fori_loop(
                0, groups, lambda n, c: merge(lb, n * group, *c), (peak, acc)
            )
        totals = acc[:, :1]
        mixed = acc[:, HD:]
        m_sq = jnp.mean(mixed * mixed, axis=-1, keepdims=True)
        normed = mixed * lax.rsqrt(m_sq + EPSILON * totals * totals)
        for h in range(heads):
            mine[lb, :, h * HD : (h + 1) * HD] = normed[h * BLOCK : (h + 1) * BLOCK].astype(BF16)
        for r in range(1, tp_n):
            tp_copy(r, lb).start()

    loads[4].wait()
    own_w = wo[pl.ds(pl.multiple_of(core * q_width, q_width), q_width), :]
    for lb in range(per_dev):
        total = jnp.dot(mine[lb], own_w, preferred_element_type=F32)
        for r in range(1, tp_n):
            tp_copy(r, lb).wait_recv()
            src = lax.rem(core - r + tp_n, tp_n)
            src_w = wo[pl.ds(pl.multiple_of(src * q_width, q_width), q_width), :]
            total = total + jnp.dot(theirs[r - 1, lb], src_w, preferred_element_type=F32)
        out_ref[lb * BLOCK : (lb + 1) * BLOCK, :] = total.astype(BF16)

    def sent(i):
        @pl.when(me + i + 1 < kv_n)
        def _():
            kv_copy(i).wait_send()

    repeat(kv_n - 1, sent)
    for lb in range(per_dev):
        for r in range(1, tp_n):
            tp_copy(r, lb).wait_send()


def on_device(kv_n, tp_n, tokens, chosen, w_query, w_key, w_value, w_out, q_gain, k_gain):
    rows, depth = tokens.shape
    q_width = w_query.shape[1]
    per_dev = rows // BLOCK
    heads = q_width // HD
    group = next(g for g in (3, 2, 1) if (kv_n - 1) % g == 0)
    vmem = pl.BlockSpec(memory_space=pltpu.VMEM)
    hbm = pl.BlockSpec(memory_space=pl.ANY)
    return pl.pallas_call(
        functools.partial(kernel, kv_n, tp_n, group),
        out_shape=jax.ShapeDtypeStruct((rows, w_out.shape[1]), BF16),
        in_specs=[vmem] * 3 + [hbm] * 5,
        out_specs=vmem,
        scratch_shapes=[
            pltpu.VMEM((rows, depth), BF16),
            pltpu.VMEM((depth, q_width), BF16),
            pltpu.VMEM((2 * HD, depth), BF16),
            pltpu.VMEM(w_out.shape, BF16),
            pltpu.VMEM((rows, 2 * HD), BF16),
            pltpu.VMEM((kv_n - 1, BLOCK, 2 * HD), BF16),
            pltpu.VMEM((kv_n - 1, BLOCK, 2 * HD), BF16),
            pltpu.VMEM((per_dev, heads * BLOCK, 2 * HD), BF16),
            pltpu.VMEM((per_dev, BLOCK, q_width), BF16),
            pltpu.VMEM((tp_n - 1, per_dev, BLOCK, q_width), BF16),
            pltpu.SemaphoreType.DMA((5,)),
            pltpu.SemaphoreType.DMA((kv_n - 1,)),
            pltpu.SemaphoreType.DMA((kv_n - 1,)),
            pltpu.SemaphoreType.DMA((tp_n - 1, per_dev)),
            pltpu.SemaphoreType.DMA((tp_n - 1, per_dev)),
        ],
        compiler_params=pltpu.CompilerParams(collective_id=0, has_side_effects=True),
    )(
        chosen, q_gain.reshape(1, HD), k_gain.reshape(1, HD),
        tokens, w_query, w_key.T, w_value.T, w_out,
    )


def solution(mesh):
    placed = (
        P(("dp", "kv"), None),
        P("dp", None),
        P(None, "tp"),
        P(None, "tp"),
        P(None, "tp"),
        P(None, "tp"),
        P(),
        P(),
    )
    return jax.shard_map(
        functools.partial(on_device, mesh.shape["kv"], mesh.shape["tp"]),
        mesh=mesh, in_specs=placed, out_specs=P(("dp", "kv"), "tp"), check_vma=False,
    )
```

```python
import functools

import jax
import jax.numpy as jnp
from jax import lax
from jax.experimental import pallas as pl
from jax.experimental.pallas import tpu as pltpu
from jax.sharding import PartitionSpec as P

HD = 64
BLOCK = 128
NEGATIVE = -1e30
EPSILON = 1e-05
MESH = pl.DeviceIdType.MESH
F32 = jnp.float32
BF16 = jnp.bfloat16


def repeat(count, body):
    if count <= 8:
        for i in range(count):
            body(i)
    else:
        lax.fori_loop(0, count, lambda i, c: (body(i), c)[1], 0)


def dot_nt(a, b):
    return lax.dot_general(a, b, (((1,), (1,)), ((), ())), preferred_element_type=F32)


def kernel(
    kv_n, tp_n, group,
    chosen_hbm, qg_hbm, kg_hbm, tok_hbm, wq_hbm, wk_hbm, wv_hbm,
    out_ref,
    chosen_ref, qg_ref, kg_ref, tok, wq, wkv, local, stage, slots, queries, mine, theirs,
    load_sem, kv_send, kv_recv, tp_send, tp_recv,
):
    me = lax.axis_index("kv")
    core = lax.axis_index("tp")
    rows = tok.shape[0]
    per_dev = rows // BLOCK
    q_width = wq.shape[1]
    heads = q_width // HD
    first = me * per_dev

    loads = [
        pltpu.make_async_copy(wk_hbm, wkv.at[pl.ds(0, HD)], load_sem.at[0]),
        pltpu.make_async_copy(wv_hbm, wkv.at[pl.ds(HD, HD)], load_sem.at[1]),
        pltpu.make_async_copy(tok_hbm, tok, load_sem.at[2]),
        pltpu.make_async_copy(chosen_hbm, chosen_ref, load_sem.at[3]),
        pltpu.make_async_copy(qg_hbm, qg_ref, load_sem.at[4]),
        pltpu.make_async_copy(kg_hbm, kg_ref, load_sem.at[5]),
        pltpu.make_async_copy(wq_hbm, wq, load_sem.at[6]),
    ]
    for load in loads:
        load.start()

    barrier = pltpu.get_barrier_semaphore()

    def greet(i):
        pl.semaphore_signal(
            barrier, inc=1, device_id={"kv": lax.rem(me + i + 1, kv_n)}, device_id_type=MESH
        )

    repeat(kv_n - 1, greet)
    for r in range(1, tp_n):
        pl.semaphore_signal(
            barrier, inc=1, device_id={"tp": lax.rem(core + r, tp_n)}, device_id_type=MESH
        )

    def found(cond):
        return jnp.max(jnp.where(cond, 1.0, 0.0), axis=(0, 1), keepdims=True)

    for load in loads[:-1]:
        load.wait()
    chosen = chosen_ref[...]
    gain_row = jnp.concatenate([qg_ref[...], qg_ref[...]], axis=1)
    q_gain = jnp.broadcast_to(gain_row, (2 * HD, 2 * HD)).T[:HD]
    queries[:, HD:, :] = jnp.zeros((per_dev, HD, heads * BLOCK), BF16)
    row_id = lax.broadcasted_iota(jnp.int32, chosen.shape, 0)
    kv = dot_nt(tok[...], wkv[...])
    lane = lax.broadcasted_iota(jnp.int32, (rows, 2 * HD), 1)
    is_key = lane < HD
    mean_sq = jnp.sum(jnp.where(is_key, kv * kv, 0.0), axis=-1, keepdims=True) * (1.0 / HD)
    gain = jnp.concatenate([kg_ref[...], jnp.ones((1, HD), F32)], axis=1)
    packed = jnp.where(is_key, kv * lax.rsqrt(mean_sq + EPSILON), kv) * gain
    local[...] = packed.astype(BF16)

    def fill(i):
        dest = me + i + 1

        @pl.when(dest < kv_n)
        def _():
            asked = (row_id >= dest * per_dev) & (row_id < (dest + 1) * per_dev)
            sel = packed[:BLOCK]
            for j in range(1, per_dev):
                hit = jnp.broadcast_to(found(asked & (chosen == first + j)), sel.shape)
                sel = jnp.where(hit > 0.5, packed[j * BLOCK : (j + 1) * BLOCK], sel)
            stage[i] = sel.astype(BF16)

        @pl.when(me - i - 1 < 0)
        def _():
            slots[i] = jnp.zeros(slots.shape[1:], BF16)

    repeat(kv_n - 1, fill)

    pl.semaphore_wait(barrier, kv_n - 1 + tp_n - 1)

    def kv_copy(i):
        return pltpu.make_async_remote_copy(
            src_ref=stage.at[i],
            dst_ref=slots.at[i],
            send_sem=kv_send.at[i],
            recv_sem=kv_recv.at[i],
            device_id={"kv": lax.rem(me + i + 1, kv_n)},
            device_id_type=MESH,
        )

    def send(i):
        far = kv_n - 2 - i

        @pl.when(me + far + 1 < kv_n)
        def _():
            kv_copy(far).start()

    repeat(kv_n - 1, send)

    loads[-1].wait()
    query = jnp.dot(tok[...], wq[...], preferred_element_type=F32)
    for pair in range(heads // 2):
        for lb in range(per_dev):
            tile = query[lb * BLOCK : (lb + 1) * BLOCK, pair * 2 * HD : (pair + 1) * 2 * HD].T
            for half in range(2):
                qh = tile[half * HD : (half + 1) * HD]
                q_sq = jnp.mean(qh * qh, axis=0, keepdims=True)
                qh = qh * lax.rsqrt(q_sq + EPSILON) * q_gain * HD**-0.5
                h = pair * 2 + half
                queries[lb, :HD, h * BLOCK : (h + 1) * BLOCK] = qh.astype(BF16)

    lane_row = lax.broadcasted_iota(jnp.int32, (1, 2 * HD), 1)
    keep = jnp.where(lane_row < HD, 0.0, 1.0).astype(BF16)
    ones = jnp.where(lane_row < HD, 1.0, 0.0).astype(BF16)

    def mix(weights, keyset):
        return lax.dot_general(
            keyset * keep + ones, weights, (((0,), (0,)), ((), ())), preferred_element_type=F32
        )

    span = heads * BLOCK
    q_pos = lax.rem(lax.broadcasted_iota(jnp.int32, (BLOCK, span), 1), BLOCK)
    causal = lax.broadcasted_iota(jnp.int32, (BLOCK, span), 0) <= q_pos

    def bias_of(cond):
        return (1.0 - found(cond)) * NEGATIVE

    def top(part):
        return jnp.max(part, axis=0, keepdims=True)

    def softmax_parts(parts, biases, peak):
        for part, bias in zip(parts, biases):
            level = top(part) if bias is None else top(part) + bias
            peak = level if peak is None else jnp.maximum(peak, level)
        weights = [
            jnp.exp(part - (peak if bias is None else peak - bias)).astype(BF16)
            for part, bias in zip(parts, biases)
        ]
        return peak, jnp.concatenate(weights, axis=0) if len(weights) > 1 else weights[0]

    state = []
    for lb in range(per_dev):
        mine_row = row_id == first + lb
        keyset = local[: (lb + 1) * BLOCK]
        scores = jnp.dot(keyset, queries[lb], preferred_element_type=F32)
        parts = [scores[j * BLOCK : (j + 1) * BLOCK] for j in range(lb + 1)]
        parts[lb] = jnp.where(causal, parts[lb], NEGATIVE)
        biases = [bias_of(mine_row & (chosen == first + j)) for j in range(lb)] + [None]
        peak, weights = softmax_parts(parts, biases, None)
        state.append((peak, mix(weights, keyset)))

    def arrive(i):
        @pl.when(me - i - 1 >= 0)
        def _():
            kv_copy(i).wait_recv()

    def merge(lb, base, peak, acc):
        mine_row = row_id == first + lb
        keyset = slots[pl.ds(base, group)].reshape(group * BLOCK, 2 * HD)
        biases = []
        for g in range(group):
            low = (me - base - g - 1) * per_dev
            biases.append(
                bias_of(mine_row & (chosen >= 0) & (chosen >= low) & (chosen < low + per_dev))
            )
        scores = jnp.dot(keyset, queries[lb], preferred_element_type=F32)
        parts = [scores[g * BLOCK : (g + 1) * BLOCK] for g in range(group)]
        peak_now, weights = softmax_parts(parts, biases, peak)
        return peak_now, acc * jnp.exp(peak - peak_now) + mix(weights, keyset)

    def tp_copy(r, lb):
        return pltpu.make_async_remote_copy(
            src_ref=mine.at[lb],
            dst_ref=theirs.at[r - 1, lb],
            send_sem=tp_send.at[r - 1, lb],
            recv_sem=tp_recv.at[r - 1, lb],
            device_id={"tp": lax.rem(core + r, tp_n)},
            device_id_type=MESH,
        )

    repeat(kv_n - 1, arrive)
    groups = (kv_n - 1) // group
    for lb in range(per_dev):
        peak, acc = state[lb]
        if groups <= 2:
            for n in range(groups):
                peak, acc = merge(lb, n * group, peak, acc)
        else:
            peak, acc = lax.fori_loop(
                0, groups, lambda n, c: merge(lb, n * group, *c), (peak, acc)
            )
        totals = acc[:1]
        mixed = acc[HD:]
        m_sq = jnp.mean(mixed * mixed, axis=0, keepdims=True)
        normed = mixed * lax.rsqrt(m_sq + EPSILON * totals * totals)
        for pair in range(heads // 2):
            both = [normed[:, h * BLOCK : (h + 1) * BLOCK] for h in (2 * pair, 2 * pair + 1)]
            both = jnp.concatenate(both, axis=0).T
            mine[lb, :, pair * 2 * HD : (pair + 1) * 2 * HD] = both.astype(BF16)
        for r in range(1, tp_n):
            tp_copy(r, lb).start()

    for lb in range(per_dev):
        block = slice(lb * BLOCK, (lb + 1) * BLOCK)
        out_ref[block, pl.ds(pl.multiple_of(core * q_width, q_width), q_width)] = mine[lb]
        for r in range(1, tp_n):
            tp_copy(r, lb).wait_recv()
            src = lax.rem(core - r + tp_n, tp_n)
            out_ref[block, pl.ds(pl.multiple_of(src * q_width, q_width), q_width)] = theirs[r - 1, lb]

    def sent(i):
        @pl.when(me + i + 1 < kv_n)
        def _():
            kv_copy(i).wait_send()

    repeat(kv_n - 1, sent)
    for lb in range(per_dev):
        for r in range(1, tp_n):
            tp_copy(r, lb).wait_send()


def on_device(kv_n, tp_n, tokens, chosen, w_query, w_key, w_value, w_out, q_gain, k_gain):
    rows, depth = tokens.shape
    q_width = w_query.shape[1]
    per_dev = rows // BLOCK
    heads = q_width // HD
    group = next(g for g in (3, 2, 1) if (kv_n - 1) % g == 0)
    vmem = pl.BlockSpec(memory_space=pltpu.VMEM)
    hbm = pl.BlockSpec(memory_space=pltpu.HBM)
    attended = pl.pallas_call(
        functools.partial(kernel, kv_n, tp_n, group),
        out_shape=pltpu.VMEM((rows, tp_n * q_width), BF16),
        in_specs=[hbm] * 7,
        out_specs=vmem,
        scratch_shapes=[
            pltpu.VMEM(chosen.shape, jnp.int32),
            pltpu.VMEM((1, HD), F32),
            pltpu.VMEM((1, HD), F32),
            pltpu.VMEM((rows, depth), BF16),
            pltpu.VMEM((depth, q_width), BF16),
            pltpu.VMEM((2 * HD, depth), BF16),
            pltpu.VMEM((rows, 2 * HD), BF16),
            pltpu.VMEM((kv_n - 1, BLOCK, 2 * HD), BF16),
            pltpu.VMEM((kv_n - 1, BLOCK, 2 * HD), BF16),
            pltpu.VMEM((per_dev, 2 * HD, heads * BLOCK), BF16),
            pltpu.VMEM((per_dev, BLOCK, q_width), BF16),
            pltpu.VMEM((tp_n - 1, per_dev, BLOCK, q_width), BF16),
            pltpu.SemaphoreType.DMA((7,)),
            pltpu.SemaphoreType.DMA((kv_n - 1,)),
            pltpu.SemaphoreType.DMA((kv_n - 1,)),
            pltpu.SemaphoreType.DMA((tp_n - 1, per_dev)),
            pltpu.SemaphoreType.DMA((tp_n - 1, per_dev)),
        ],
        compiler_params=pltpu.CompilerParams(
            collective_id=0, has_side_effects=True,
        ),
    )(
        chosen, q_gain.reshape(1, HD), k_gain.reshape(1, HD),
        tokens, w_query, w_key.T, w_value.T,
    )
    return jnp.dot(attended, w_out, preferred_element_type=F32).astype(BF16)


def solution(mesh):
    placed = (
        P(("dp", "kv"), None),
        P("dp", None),
        P(None, "tp"),
        P(None, "tp"),
        P(None, "tp"),
        P(None, "tp"),
        P(),
        P(),
    )
    return jax.shard_map(
        functools.partial(on_device, mesh.shape["kv"], mesh.shape["tp"]),
        mesh=mesh, in_specs=placed, out_specs=P(("dp", "kv"), "tp"), check_vma=False,
    )
```

```python
import functools

import jax
import jax.numpy as jnp
from jax import lax
from jax.experimental import pallas as pl
from jax.experimental.pallas import tpu as pltpu
from jax.sharding import PartitionSpec as P

HD = 64
BLOCK = 128
NEGATIVE = -1e30
EPSILON = 1e-05
MESH = pl.DeviceIdType.MESH
F32 = jnp.float32
BF16 = jnp.bfloat16


def repeat(count, body):
    if count <= 8:
        for i in range(count):
            body(i)
    else:
        lax.fori_loop(0, count, lambda i, c: (body(i), c)[1], 0)


def dot_nt(a, b):
    return lax.dot_general(a, b, (((1,), (1,)), ((), ())), preferred_element_type=F32)


def kernel(
    kv_n, tp_n, group,
    chosen_hbm, qg_hbm, kg_hbm, tok_hbm, wq_hbm, wk_hbm, wv_hbm,
    out_ref,
    chosen_ref, qg_ref, kg_ref, tok, wq, wkv, local, stage, slots, queries, mine, theirs,
    load_sem, kv_send, kv_recv, tp_send, tp_recv,
):
    me = lax.axis_index("kv")
    core = lax.axis_index("tp")
    rows = tok.shape[0]
    per_dev = rows // BLOCK
    q_width = wq.shape[1]
    heads = q_width // HD
    first = me * per_dev

    loads = [
        pltpu.make_async_copy(chosen_hbm, chosen_ref, load_sem.at[0]),
        pltpu.make_async_copy(qg_hbm, qg_ref, load_sem.at[1]),
        pltpu.make_async_copy(kg_hbm, kg_ref, load_sem.at[2]),
        pltpu.make_async_copy(wk_hbm, wkv.at[pl.ds(0, HD)], load_sem.at[3]),
        pltpu.make_async_copy(wv_hbm, wkv.at[pl.ds(HD, HD)], load_sem.at[4]),
        pltpu.make_async_copy(tok_hbm, tok, load_sem.at[5]),
        pltpu.make_async_copy(wq_hbm, wq, load_sem.at[6]),
    ]

    barrier = pltpu.get_barrier_semaphore()

    def greet(i):
        @pl.when(me - i - 1 >= 0)
        def _():
            pl.semaphore_signal(
                barrier, inc=1, device_id={"kv": me - i - 1}, device_id_type=MESH
            )

    repeat(kv_n - 1, greet)
    for r in range(1, tp_n):
        pl.semaphore_signal(
            barrier, inc=1, device_id={"tp": lax.rem(core + r, tp_n)}, device_id_type=MESH
        )

    for load in loads[:-1]:
        load.start()

    def found(cond):
        return jnp.max(jnp.where(cond, 1.0, 0.0), axis=(0, 1), keepdims=True)

    for load in loads[:3]:
        load.wait()
    chosen = chosen_ref[...]
    row_id = lax.broadcasted_iota(jnp.int32, chosen.shape, 0)

    def column(gain):
        row = jnp.concatenate([gain, gain], axis=1)
        return jnp.broadcast_to(row, (2 * HD, 2 * HD)).T[:HD]

    q_gain = column(qg_ref[...])
    k_gain = column(kg_ref[...])
    short = kv_n <= 9

    def wants(i, j):
        dest = me + i + 1
        asked = (row_id >= dest * per_dev) & (row_id < (dest + 1) * per_dev)
        return found(asked & (chosen == first + j))

    def remote_bias(lb, i):
        low = (me - i - 1) * per_dev
        live = (chosen >= 0) & (chosen >= low) & (chosen < low + per_dev)
        return (1.0 - found((row_id == first + lb) & live)) * NEGATIVE

    wanted = [[wants(i, j) for j in range(1, per_dev)] for i in range(kv_n - 1)] if short else None
    remote_biases = (
        [[remote_bias(lb, i) for i in range(kv_n - 1)] for lb in range(per_dev)] if short else None
    )
    local_biases = [
        [(1.0 - found((row_id == first + lb) & (chosen == first + j))) * NEGATIVE for j in range(lb)]
        for lb in range(per_dev)
    ]

    for load in loads[3:-1]:
        load.wait()
    loads[-1].start()
    kv = dot_nt(wkv[...], tok[...])
    keys = kv[:HD]
    mean_sq = jnp.mean(keys * keys, axis=0, keepdims=True)
    keys = keys * lax.rsqrt(mean_sq + EPSILON)
    packed = []
    for j in range(per_dev):
        block = slice(j * BLOCK, (j + 1) * BLOCK)
        packed.append(jnp.concatenate([keys[:, block] * k_gain, kv[HD:, block]], axis=0))
        local[j] = packed[j].astype(BF16)

    def fill(i):
        dest = me + i + 1

        @pl.when(dest < kv_n)
        def _():
            sel = packed[0]
            for j in range(1, per_dev):
                hit = wanted[i][j - 1] if short else wants(i, j)
                hit = jnp.broadcast_to(hit, sel.shape)
                sel = jnp.where(hit > 0.5, packed[j], sel)
            stage[i] = sel.astype(BF16)

        @pl.when(me - i - 1 < 0)
        def _():
            slots[i] = jnp.zeros(slots.shape[1:], BF16)

    repeat(kv_n - 1, fill)

    pl.semaphore_wait(barrier, kv_n - 1 - me + tp_n - 1)

    def kv_copy(i, part):
        half = pl.ds(part * HD, HD)
        return pltpu.make_async_remote_copy(
            src_ref=stage.at[i, half],
            dst_ref=slots.at[i, half],
            send_sem=kv_send.at[part, i],
            recv_sem=kv_recv.at[part, i],
            device_id={"kv": lax.rem(me + i + 1, kv_n)},
            device_id_type=MESH,
        )

    def send(part, i):
        @pl.when(me + i + 1 < kv_n)
        def _():
            kv_copy(i, part).start()

    repeat(kv_n - 1, functools.partial(send, 0))
    repeat(kv_n - 1, functools.partial(send, 1))

    loads[-1].wait()
    query = jnp.dot(tok[...], wq[...], preferred_element_type=F32)
    for pair in range(heads // 2):
        for lb in range(per_dev):
            tile = query[lb * BLOCK : (lb + 1) * BLOCK, pair * 2 * HD : (pair + 1) * 2 * HD].T
            for half in range(2):
                qh = tile[half * HD : (half + 1) * HD]
                q_sq = jnp.mean(qh * qh, axis=0, keepdims=True)
                qh = qh * lax.rsqrt(q_sq + EPSILON) * q_gain * HD**-0.5
                h = pair * 2 + half
                queries[lb, :, h * BLOCK : (h + 1) * BLOCK] = qh.astype(BF16)

    def mix(weights, values):
        values = jnp.concatenate(values, axis=1) if len(values) > 1 else values[0]
        weights = jnp.concatenate(weights, axis=0) if len(weights) > 1 else weights[0]
        ones = jnp.ones((HD, values.shape[1]), BF16)
        return jnp.dot(
            jnp.concatenate([ones, values], axis=0), weights, preferred_element_type=F32
        )

    def scores_of(keyset, lb):
        return lax.dot_general(
            keyset, queries[lb], (((0,), (0,)), ((), ())), preferred_element_type=F32
        )

    span = heads * BLOCK
    q_pos = lax.rem(lax.broadcasted_iota(jnp.int32, (BLOCK, span), 1), BLOCK)
    causal = lax.broadcasted_iota(jnp.int32, (BLOCK, span), 0) <= q_pos

    def top(part):
        return jnp.max(part, axis=0, keepdims=True)

    def softmax_parts(parts, biases, peak):
        for part, bias in zip(parts, biases):
            level = top(part) if bias is None else top(part) + bias
            peak = level if peak is None else jnp.maximum(peak, level)
        weights = [
            jnp.exp(part - (peak if bias is None else peak - bias)).astype(BF16)
            for part, bias in zip(parts, biases)
        ]
        return peak, weights

    state = []
    for lb in range(per_dev):
        parts = [scores_of(local[j, :HD], lb) for j in range(lb + 1)]
        parts[lb] = jnp.where(causal, parts[lb], NEGATIVE)
        biases = local_biases[lb] + [None]
        peak, weights = softmax_parts(parts, biases, None)
        state.append((peak, mix(weights, [local[j, HD:] for j in range(lb + 1)])))

    def arrive(part, i):
        @pl.when(me - i - 1 >= 0)
        def _():
            kv_copy(i, part).wait_recv()

    def weigh(lb, base, peak):
        parts = [scores_of(slots[base + g, :HD], lb) for g in range(group)]
        biases = [
            remote_biases[lb][base + g] if short else remote_bias(lb, base + g)
            for g in range(group)
        ]
        return softmax_parts(parts, biases, peak)

    def add(base, before, peak, weights, acc):
        return acc * jnp.exp(before - peak) + mix(
            weights, [slots[base + g, HD:] for g in range(group)]
        )

    def merge(lb, n, carry):
        before, acc = carry
        peak, weights = weigh(lb, n * group, before)
        return peak, add(n * group, before, peak, weights, acc)

    def tp_copy(r, lb):
        return pltpu.make_async_remote_copy(
            src_ref=mine.at[lb],
            dst_ref=theirs.at[r - 1, lb],
            send_sem=tp_send.at[r - 1, lb],
            recv_sem=tp_recv.at[r - 1, lb],
            device_id={"tp": lax.rem(core + r, tp_n)},
            device_id_type=MESH,
        )

    groups = (kv_n - 1) // group
    single = short and groups == 1
    repeat(kv_n - 1, functools.partial(arrive, 0))
    if single:
        weighed = [weigh(lb, 0, state[lb][0]) for lb in range(per_dev)]
    repeat(kv_n - 1, functools.partial(arrive, 1))
    for lb in range(per_dev):
        before, acc = state[lb]
        if single:
            acc = add(0, before, *weighed[lb], acc)
        else:
            _, acc = lax.fori_loop(0, groups, functools.partial(merge, lb), state[lb])
        totals = acc[:1]
        mixed = acc[HD:]
        m_sq = jnp.mean(mixed * mixed, axis=0, keepdims=True)
        normed = mixed * lax.rsqrt(m_sq + EPSILON * totals * totals)
        for pair in range(heads // 2):
            both = [normed[:, h * BLOCK : (h + 1) * BLOCK] for h in (2 * pair, 2 * pair + 1)]
            both = jnp.concatenate(both, axis=0).T
            mine[lb, :, pair * 2 * HD : (pair + 1) * 2 * HD] = both.astype(BF16)
        for r in range(1, tp_n):
            tp_copy(r, lb).start()

    for lb in range(per_dev):
        block = slice(lb * BLOCK, (lb + 1) * BLOCK)
        out_ref[block, pl.ds(pl.multiple_of(core * q_width, q_width), q_width)] = mine[lb]
        for r in range(1, tp_n):
            tp_copy(r, lb).wait_recv()
            src = lax.rem(core - r + tp_n, tp_n)
            out_ref[block, pl.ds(pl.multiple_of(src * q_width, q_width), q_width)] = theirs[r - 1, lb]

    def sent(i):
        @pl.when(me + i + 1 < kv_n)
        def _():
            kv_copy(i, 0).wait_send()
            kv_copy(i, 1).wait_send()

    repeat(kv_n - 1, sent)
    for lb in range(per_dev):
        for r in range(1, tp_n):
            tp_copy(r, lb).wait_send()


def on_device(kv_n, tp_n, tokens, chosen, w_query, w_key, w_value, w_out, q_gain, k_gain):
    rows, depth = tokens.shape
    q_width = w_query.shape[1]
    per_dev = rows // BLOCK
    heads = q_width // HD
    group = next(g for g in (3, 2, 1) if (kv_n - 1) % g == 0)
    vmem = pl.BlockSpec(memory_space=pltpu.VMEM)
    hbm = pl.BlockSpec(memory_space=pltpu.HBM)
    attended = pl.pallas_call(
        functools.partial(kernel, kv_n, tp_n, group),
        out_shape=pltpu.VMEM((rows, tp_n * q_width), BF16),
        in_specs=[hbm] * 7,
        out_specs=vmem,
        scratch_shapes=[
            pltpu.VMEM(chosen.shape, jnp.int32),
            pltpu.VMEM((1, HD), F32),
            pltpu.VMEM((1, HD), F32),
            pltpu.VMEM((rows, depth), BF16),
            pltpu.VMEM((depth, q_width), BF16),
            pltpu.VMEM((2 * HD, depth), BF16),
            pltpu.VMEM((per_dev, 2 * HD, BLOCK), BF16),
            pltpu.VMEM((kv_n - 1, 2 * HD, BLOCK), BF16),
            pltpu.VMEM((kv_n - 1, 2 * HD, BLOCK), BF16),
            pltpu.VMEM((per_dev, HD, heads * BLOCK), BF16),
            pltpu.VMEM((per_dev, BLOCK, q_width), BF16),
            pltpu.VMEM((tp_n - 1, per_dev, BLOCK, q_width), BF16),
            pltpu.SemaphoreType.DMA((7,)),
            pltpu.SemaphoreType.DMA((2, kv_n - 1)),
            pltpu.SemaphoreType.DMA((2, kv_n - 1)),
            pltpu.SemaphoreType.DMA((tp_n - 1, per_dev)),
            pltpu.SemaphoreType.DMA((tp_n - 1, per_dev)),
        ],
        compiler_params=pltpu.CompilerParams(
            collective_id=0, has_side_effects=True,
        ),
    )(
        chosen, q_gain.reshape(1, HD), k_gain.reshape(1, HD),
        tokens, w_query, w_key.T, w_value.T,
    )
    return jnp.dot(attended, w_out, preferred_element_type=F32).astype(BF16)


def solution(mesh):
    placed = (
        P(("dp", "kv"), None),
        P("dp", None),
        P(None, "tp"),
        P(None, "tp"),
        P(None, "tp"),
        P(None, "tp"),
        P(),
        P(),
    )
    return jax.shard_map(
        functools.partial(on_device, mesh.shape["kv"], mesh.shape["tp"]),
        mesh=mesh, in_specs=placed, out_specs=P(("dp", "kv"), "tp"), check_vma=False,
    )
```
